128 devices in a mesh: kv: 16 (over z, y), tp: 8 (over x, core).
Axes of the slice: x: 4, y: 4, z: 4, core: 2. Of those that a mesh axis runs over, the one named last changes fastest.
Arguments:
- hidden_in: bfloat16 [16, 4096], P(None, ('kv', 'tp')), may hold values from -12 to 12
- attn_gain: float32 [4096], P('kv'), may hold values from 0.1 to 1.9
- query_weight: bfloat16 [4096, 4096], P('kv', 'tp'), may hold values from -0.09375 to 0.09375
- key_cache: bfloat16 [16, 16384, 8, 128], P(None, 'kv', 'tp'), may hold values from -600 to 600
- value_cache: bfloat16 [16, 16384, 8, 128], P(None, 'kv', 'tp'), may hold values from -6 to 6
- lambdas: float32 [32], P('tp'), may hold values from 0.3 to 0.8
- head_gain: float32 [128], replicated, may hold values from 0.1 to 1.9
- out_weight: bfloat16 [4096, 4096], P('tp', 'kv'), may hold values from -0.09375 to 0.09375
- mixer_gain: float32 [4096], P(('kv', 'tp')), may hold values from 0.1 to 1.9
- gate_weight: bfloat16 [4096, 11264], P('kv', 'tp'), may hold values from -0.09375 to 0.09375
- up_weight: bfloat16 [4096, 11264], P('kv', 'tp'), may hold values from -0.09375 to 0.09375
- down_weight: bfloat16 [11264, 4096], P('tp', 'kv'), may hold values from -0.0546875 to 0.0546875
Outputs:
- mixed: bfloat16 [16, 4096], P(None, ('kv', 'tp'))
The draws below stay inside these ranges and needn't reach their ends.
All inputs are finite; a program needn't handle non-finite values.
Results may differ from the reference program's by a relative error of at most 0.017.
Values may be sent and summed in bfloat16 or wider, within the bound.
A program may use at most 64 MiB of HBM per device.

```python
import jax
import jax.numpy as jnp
from jax import lax

D = 4096
FF = 11264
HEAD_DIM = 64
KV_HEADS = 8
GROUP = 4
HEADS = 32
BATCH = 16
LENGTH = 16384
COLS_DEV = 32
N_TP = 8


def draw_hidden_in(key, part):
    first = jax.random.fold_in(key, 11)
    second = jax.random.fold_in(key, 12)
    blocks = D // COLS_DEV
    ramp = jnp.arange(blocks, dtype=jnp.float32) / max(blocks - 1, 1)
    jitter = jax.random.uniform(second, (blocks,), jnp.float32, -0.15, 0.15)
    block_scale = jnp.exp(jnp.log(0.5) + ramp * jnp.log(6.0) + jitter)
    base = jax.random.normal(first, (BATCH, D), jnp.float32)
    column_scale = jnp.repeat(block_scale, COLS_DEV)
    values = jnp.clip(base * column_scale[None, :], -12.0, 12.0)
    return values.astype(jnp.bfloat16)


def draw_key_cache(key, part):
    first = jax.random.fold_in(key, 21)
    base = 2.0 * jnp.clip(jax.random.normal(first, (BATCH, LENGTH, KV_HEADS, 2 * HEAD_DIM), jnp.float32), -6.0, 6.0)
    return jnp.clip(base, -600.0, 600.0).astype(jnp.bfloat16)


def level_of(stream_key, shape, pieces, least, top_value):
    level, own = 1.0, jax.random.fold_in(stream_key, 6)
    for axis_at, shards_of in pieces:
        steps = jnp.exp(jax.random.uniform(jax.random.fold_in(own, axis_at), (shards_of,), jnp.float32, least / len(pieces), top_value / len(pieces)))
        level = level * jnp.repeat(steps, shape[axis_at] // shards_of).reshape([-1 if axis == axis_at else 1 for axis in range(len(shape))])
    return level


def centred(rng, shape, scale, reach, pieces=(), held_as=jnp.bfloat16):
    result = scale * jax.random.normal(rng, shape, jnp.float32)
    if pieces:
        result = result * level_of(rng, shape, pieces, -0.22, 0.18)
    return jnp.clip(result, -reach, reach).astype(held_as)


def setup_inputs(seed: int = 0) -> dict:
    arg_keys = jax.random.split(jax.random.key(seed), 13)
    hidden_in = draw_hidden_in(jax.random.fold_in(arg_keys[12], 71), 0)
    attn_gain = jnp.clip(1.0 + 0.18 * jax.random.normal(arg_keys[1], (D,), jnp.float32), 0.1, 1.9)
    query_weight = centred(arg_keys[2], (D, HEADS * 2 * HEAD_DIM), D ** -0.5, 0.09375, ((0, 16), (1, 8)))
    key_cache = draw_key_cache(jax.random.fold_in(arg_keys[12], 71), 0)
    value_cache = centred(arg_keys[4], (BATCH, LENGTH, KV_HEADS, 2 * HEAD_DIM), 1.0, 6.0, ((1, 16), (2, 8)))
    lambdas = jnp.clip(0.3 + 0.5 * jax.random.uniform(arg_keys[5], (HEADS,), jnp.float32) ** level_of(arg_keys[5], (HEADS,), ((0, 8),), -0.2, 0.2), 0.3, 0.8)
    head_gain = jnp.clip(1.0 + 0.18 * jax.random.normal(arg_keys[6], (2 * HEAD_DIM,), jnp.float32), 0.1, 1.9)
    out_weight = centred(arg_keys[7], (HEADS * 2 * HEAD_DIM, D), (HEADS * 2 * HEAD_DIM) ** -0.5, 0.09375, ((0, 8), (1, 16)))
    mixer_gain = jnp.clip(1.0 + 0.18 * jax.random.normal(arg_keys[8], (D,), jnp.float32), 0.1, 1.9)
    gate_weight = centred(arg_keys[9], (D, FF), D ** -0.5, 0.09375, ((0, 16), (1, 8)))
    up_weight = centred(arg_keys[10], (D, FF), D ** -0.5, 0.09375, ((0, 16), (1, 8)))
    down_weight = centred(arg_keys[11], (FF, D), FF ** -0.5, 0.0546875, ((0, 8), (1, 16)))
    return {"hidden_in": hidden_in, "attn_gain": attn_gain, "query_weight": query_weight, "key_cache": key_cache, "value_cache": value_cache, "lambdas": lambdas, "head_gain": head_gain, "out_weight": out_weight, "mixer_gain": mixer_gain, "gate_weight": gate_weight, "up_weight": up_weight, "down_weight": down_weight}


eps = 1e-06

def split_sum(activations, weights):
    block_rows = activations.shape[1] // N_TP
    partials = jnp.einsum('bjr,jrd->jbd', activations.reshape(activations.shape[0], N_TP, block_rows).astype(jnp.float32), weights.reshape(N_TP, block_rows, weights.shape[1]).astype(jnp.float32))
    rounded = lax.optimization_barrier(partials.astype(jnp.bfloat16)).astype(jnp.float32)
    return lax.optimization_barrier(jnp.sum(rounded, axis=0))

def reference(hidden_in, attn_gain, query_weight, key_cache, value_cache, lambdas, head_gain, out_weight, mixer_gain, gate_weight, up_weight, down_weight):
    rows_f = hidden_in.astype(jnp.float32)
    inverse = lax.rsqrt(lax.optimization_barrier(jnp.mean(rows_f * rows_f, axis=1, keepdims=True)) + eps)
    gained = (rows_f * attn_gain).astype(jnp.bfloat16)
    query_full = (jnp.dot(gained, query_weight, preferred_element_type=jnp.float32) * inverse).astype(jnp.bfloat16)
    query_heads = query_full.reshape(BATCH, KV_HEADS, GROUP, 2, HEAD_DIM)
    mixing = lambdas.reshape(KV_HEADS, GROUP)

    def one_group(group_index):
        query_part = lax.dynamic_index_in_dim(query_heads, group_index, 1, keepdims=False).astype(jnp.float32)
        key_part = lax.dynamic_index_in_dim(key_cache, group_index, 2, keepdims=False).astype(jnp.float32)
        key_part = key_part.reshape(BATCH, LENGTH, 2, HEAD_DIM)
        value_part = lax.dynamic_index_in_dim(value_cache, group_index, 2, keepdims=False).astype(jnp.float32)
        scores = jnp.einsum('bgcd,blcd->cbgl', query_part, key_part) * HEAD_DIM ** (-0.5)
        maxima = lax.optimization_barrier(jnp.max(scores, axis=-1, keepdims=True))
        exponent = jnp.exp(scores - maxima)
        totals = lax.optimization_barrier(jnp.sum(exponent, axis=-1))
        rounded = lax.optimization_barrier(exponent.astype(jnp.bfloat16)).astype(jnp.float32)
        weighted = jnp.einsum('cbgl,bld->cbgd', rounded, value_part)
        head_means = weighted / totals[..., None]
        lam_row = lax.dynamic_index_in_dim(mixing, group_index, 0, keepdims=False)
        attended = head_means[0] - lam_row[None, :, None] * head_means[1]
        norm_inv = lax.rsqrt(lax.optimization_barrier(jnp.mean(attended * attended, axis=-1, keepdims=True)) + eps)
        return (attended * norm_inv * head_gain).astype(jnp.bfloat16)
    per_group = lax.map(one_group, jnp.arange(KV_HEADS, dtype=jnp.int32))
    head_out = jnp.moveaxis(per_group, 0, 1).reshape(BATCH, HEADS * 2 * HEAD_DIM)
    attn_out = split_sum(head_out, out_weight)
    after_attn = (rows_f + attn_out).astype(jnp.bfloat16)
    after_f = after_attn.astype(jnp.float32)
    inverse_two = lax.rsqrt(lax.optimization_barrier(jnp.mean(after_f * after_f, axis=1, keepdims=True)) + eps)
    mixer_in = (after_f * inverse_two * mixer_gain).astype(jnp.bfloat16)
    gate_sum = jnp.dot(mixer_in, gate_weight, preferred_element_type=jnp.float32)
    up_sum = jnp.dot(mixer_in, up_weight, preferred_element_type=jnp.float32)
    hidden = (jax.nn.silu(gate_sum) * up_sum).astype(jnp.bfloat16)
    mixer_out = split_sum(hidden, down_weight)
    return (after_f + mixer_out).astype(jnp.bfloat16)
```

```python
import functools

import jax
import jax.numpy as jnp
from jax import lax
from jax.experimental import pallas as pl
from jax.experimental.pallas import tpu as pltpu
from jax.sharding import PartitionSpec as P

MESH = pl.DeviceIdType.MESH
F32, BF16 = jnp.float32, jnp.bfloat16

D = 4096
HEAD_DIM = 64
EPS = 1e-06

KV_OFFSETS = sorted(range(1, 16), key=lambda d: -(min(d // 4, 4 - d // 4) + min(d % 4, 4 - d % 4)))
TP_OFFSETS = sorted(range(1, 8), key=lambda d: -min(d // 2, 4 - d // 2))


def kernel(
    hid_hbm, ag_hbm, wq_hbm, k_hbm, v_hbm, lam_hbm, hg_hbm, wo_hbm, mg_hbm, wg_hbm, wu_hbm, wd_hbm,
    out_ref,
    hid, ag, wq, kc, vc, lam, hg, wo, mg, wg, wu, wd,
    g1, g1m, s2, r2, a3, s4, r4, a5, f5, a6, s7, r7, a8, f8, s9, r9,
    load_sem, send_sem, recv_sem,
):
    kv, tp = lax.axis_index("kv"), lax.axis_index("tp")
    z, y, x, core = kv // 4, kv % 4, tp // 2, tp % 2

    def kv_peer(d):
        return ((z + d // 4) % 4) * 4 + (y + d % 4) % 4

    def tp_peer(d):
        return ((x + d // 2) % 4) * 2 + (core + d % 2) % 2

    loads = [
        pltpu.make_async_copy(src, dst, load_sem.at[n])
        for n, (src, dst) in enumerate([
            (hid_hbm, hid), (mg_hbm, mg), (ag_hbm, ag), (wq_hbm, wq), (k_hbm, kc), (v_hbm, vc),
            (lam_hbm, lam), (hg_hbm, hg), (wo_hbm, wo), (wg_hbm, wg), (wu_hbm, wu), (wd_hbm, wd),
        ])
    ]
    L_HID, L_MG, L_AG, L_WQ, L_K, L_V, L_LAM, L_HG, L_WO, L_WG, L_WU, L_WD = loads
    for load in loads:
        load.start()

    barrier = pltpu.get_barrier_semaphore()
    for d in KV_OFFSETS:
        pl.semaphore_signal(barrier, inc=1, device_id={"kv": kv_peer(d), "tp": tp}, device_id_type=MESH)
    for d in TP_OFFSETS:
        pl.semaphore_signal(barrier, inc=1, device_id={"kv": kv, "tp": tp_peer(d)}, device_id_type=MESH)

    def to_kv(phase, src, dst):
        for d in KV_OFFSETS:
            peer = kv_peer(d)
            pltpu.make_async_remote_copy(
                src(peer, d), dst(peer, d), send_sem.at[phase], recv_sem.at[phase],
                device_id={"kv": peer, "tp": tp}, device_id_type=MESH,
            ).start()

    def to_tp(phase, src, dst):
        for d in TP_OFFSETS:
            peer = tp_peer(d)
            pltpu.make_async_remote_copy(
                src(peer, d), dst(peer, d), send_sem.at[phase], recv_sem.at[phase],
                device_id={"kv": kv, "tp": peer}, device_id_type=MESH,
            ).start()

    def wait_bytes(ref, sem):
        pltpu.make_async_copy(ref, ref, sem).wait()

    L_HID.wait()
    L_MG.wait()
    lane = lax.broadcasted_iota(jnp.int32, (16, 128), 1)
    mine = lane // 32 == tp % 4
    h32 = hid[...].astype(F32)
    g1[tp] = jnp.where(mine, jnp.concatenate([h32] * 4, axis=1), 0.0).astype(BF16)
    g1m[tp] = jnp.where(mine[0:1], jnp.concatenate([mg[...]] * 4, axis=1), 0.0)

    pl.semaphore_wait(barrier, 22)

    to_tp(0, lambda peer, d: g1.at[tp], lambda peer, d: g1.at[tp])
    to_tp(9, lambda peer, d: g1m.at[tp], lambda peer, d: g1m.at[tp])
    L_AG.wait()
    L_WQ.wait()
    wait_bytes(g1.at[pl.ds(0, 7)], recv_sem.at[0])
    hid_f = jnp.concatenate([sum(g1[n].astype(F32) for n in range(h, h + 4)) for h in (0, 4)], axis=1)
    squares = jnp.sum(hid_f * hid_f, axis=1, keepdims=True)
    gained = (hid_f * ag[...]).astype(BF16)
    partial = jnp.dot(gained, wq[...], preferred_element_type=F32)
    for c in range(4):
        s2[pl.ds(c, 16, stride=8), :] = partial[:, 128 * c : 128 * (c + 1)]
    s2[pl.ds(4, 16, stride=8), :] = jnp.broadcast_to(squares, (16, 128))

    to_kv(1, lambda peer, d: s2.at[pl.ds(pl.multiple_of(peer * 8, 8), 8)], lambda peer, d: r2.at[pl.ds(8 * d, 8)])
    own = s2[pl.ds(pl.multiple_of(kv * 8, 8), 8), :]
    wait_bytes(r2.at[pl.ds(0, 120)], recv_sem.at[1])
    tot = own + sum(r2[8 * d : 8 * d + 8, :] for d in range(1, 16))
    inv = lax.rsqrt(tot[4:5] / D + EPS)
    q4 = (tot[0:4] * inv).astype(BF16).astype(F32)
    low = lane[0:4] < HEAD_DIM
    a3[kv] = jnp.concatenate([jnp.where(low, q4, 0.0), jnp.where(low, 0.0, q4)], axis=0).astype(BF16)

    to_kv(2, lambda peer, d: a3.at[kv], lambda peer, d: a3.at[kv])
    L_K.wait()
    L_V.wait()
    wait_bytes(a3.at[pl.ds(0, 15)], recv_sem.at[2])

    upper = lax.broadcasted_iota(jnp.int32, (16, 128), 0) < 8

    def pair(p, _):
        both = jnp.concatenate([a3[2 * p].astype(F32), a3[2 * p + 1].astype(F32)], axis=0)
        lhs = jnp.concatenate([jnp.where(upper, both, 0.0), jnp.where(upper, 0.0, both)], axis=1).astype(BF16)
        keys = jnp.concatenate([kc[2 * p], kc[2 * p + 1]], axis=1)
        scores = lax.dot_general(lhs, keys, (((1,), (1,)), ((), ())), preferred_element_type=F32) * HEAD_DIM**-0.5
        top = jnp.max(scores, axis=1, keepdims=True)
        exponent = jnp.exp(scores - top)
        total = jnp.sum(exponent, axis=1, keepdims=True)
        values = jnp.concatenate([vc[2 * p], vc[2 * p + 1]], axis=1)
        acc = jnp.dot(exponent.astype(BF16), values, preferred_element_type=F32)
        stats = jnp.where(lane < 64, top, total)
        row = pl.multiple_of(p * 32, 32)
        s4[pl.ds(row, 8), :] = acc[0:8, 0:128]
        s4[pl.ds(row + 8, 8), :] = stats[0:8]
        s4[pl.ds(row + 16, 8), :] = acc[8:16, 128:256]
        s4[pl.ds(row + 24, 8), :] = stats[8:16]
        return 0

    lax.fori_loop(0, 8, pair, 0)

    to_kv(3, lambda peer, d: s4.at[pl.ds(pl.multiple_of(peer * 16, 16), 16)], lambda peer, d: r4.at[pl.ds(16 * d, 16)])
    L_LAM.wait()
    L_HG.wait()
    row8 = lax.broadcasted_iota(jnp.int32, (8, 128), 0)
    lane8 = lane[0:8]
    mixing = jnp.sum(jnp.where(row8 == lane8, jnp.concatenate([lam[...], jnp.zeros((1, 124), F32)], axis=1), 0.0), axis=1, keepdims=True)
    own_acc = s4[pl.ds(pl.multiple_of(kv * 16, 16), 8), :]
    own_stats = s4[pl.ds(pl.multiple_of(kv * 16 + 8, 8), 8), :]
    wait_bytes(r4.at[pl.ds(0, 240)], recv_sem.at[3])
    accs = [own_acc] + [r4[16 * d : 16 * d + 8, :] for d in range(1, 16)]
    stats = [own_stats] + [r4[16 * d + 8 : 16 * d + 16, :] for d in range(1, 16)]
    top = functools.reduce(jnp.maximum, stats)
    own_tot, own_sum = 0.0, 0.0
    for a, s in zip(accs, stats):
        factor = jnp.exp(jnp.where(lane8 < 64, s - top, 0.0))
        factor = jnp.where(lane8 < 64, factor, pltpu.roll(factor, 64, axis=1))
        own_sum += a * factor
        own_tot += s * factor
    own_tot = jnp.where(lane8 < 64, pltpu.roll(own_tot, 64, axis=1), own_tot)
    means = own_sum / own_tot
    attended = means - mixing * pltpu.roll(means, 4, axis=0)
    norm_inv = lax.rsqrt(jnp.mean(attended * attended, axis=1, keepdims=True) + EPS)
    a5[kv] = (attended * norm_inv * hg[...]).astype(BF16)

    to_kv(4, lambda peer, d: a5.at[kv], lambda peer, d: a5.at[kv])
    L_WO.wait()
    wait_bytes(a5.at[pl.ds(0, 15)], recv_sem.at[4])
    for b in range(16):
        f5[8 * b : 8 * b + 8, :] = a5[b].astype(F32)
    head_out = jnp.concatenate([f5[pl.ds(c, 16, stride=8), :] for c in range(4)], axis=1).astype(BF16)
    a6[tp] = jnp.dot(head_out, wo[...], preferred_element_type=F32).astype(BF16)

    to_tp(5, lambda peer, d: a6.at[tp], lambda peer, d: a6.at[tp])
    wait_bytes(g1m.at[pl.ds(0, 7)], recv_sem.at[9])
    gain2 = jnp.concatenate([sum(g1m[n] for n in range(h, h + 4)) for h in (0, 4)], axis=1)
    L_WG.wait()
    L_WU.wait()
    wait_bytes(a6.at[pl.ds(0, 7)], recv_sem.at[5])
    after_f = (hid_f + sum(a6[n].astype(F32) for n in range(8))).astype(BF16).astype(F32)
    squares2 = jnp.sum(after_f * after_f, axis=1, keepdims=True)
    gained2 = (after_f * gain2).astype(BF16)
    gate = jnp.dot(gained2, wg[...], preferred_element_type=F32)
    for c in range(11):
        s7[pl.ds(c, 16, stride=24), :] = gate[:, 128 * c : 128 * (c + 1)]
    up = jnp.dot(gained2, wu[...], preferred_element_type=F32)
    for c in range(11):
        s7[pl.ds(11 + c, 16, stride=24), :] = up[:, 128 * c : 128 * (c + 1)]
    s7[pl.ds(22, 16, stride=24), :] = jnp.broadcast_to(squares2, (16, 128))

    to_kv(6, lambda peer, d: s7.at[pl.ds(pl.multiple_of(peer * 24, 8), 24)], lambda peer, d: r7.at[pl.ds(24 * d, 24)])
    own = s7[pl.ds(pl.multiple_of(kv * 24, 8), 24), :]
    wait_bytes(r7.at[pl.ds(0, 360)], recv_sem.at[6])
    tot = own + sum(r7[24 * d : 24 * d + 24, :] for d in range(1, 16))
    inv2 = lax.rsqrt(tot[22:23] / D + EPS)
    tot = tot * inv2
    gate_sum, up_sum = tot[0:16], jnp.concatenate([tot[11:22], tot[0:5]], axis=0)
    a8[kv] = (gate_sum / (1.0 + jnp.exp(-gate_sum)) * up_sum).astype(BF16)

    to_kv(7, lambda peer, d: a8.at[kv], lambda peer, d: a8.at[kv])
    L_WD.wait()
    wait_bytes(a8.at[pl.ds(0, 15)], recv_sem.at[7])
    for b in range(16):
        f8[16 * b : 16 * b + 16, :] = a8[b].astype(F32)
    hidden = jnp.concatenate([f8[pl.ds(c, 16, stride=16), :] for c in range(11)], axis=1).astype(BF16)
    down = jnp.dot(hidden, wd[...], preferred_element_type=F32).astype(BF16)
    s9[0] = down[:, 0:128]
    s9[1] = down[:, 128:256]

    to_tp(8, lambda peer, d: s9.at[peer // 4], lambda peer, d: r9.at[d])
    own = s9[tp // 4].astype(F32)
    after_own = jnp.where(tp // 4 == 0, after_f[:, 0:128], after_f[:, 128:256])
    wait_bytes(r9.at[pl.ds(0, 7)], recv_sem.at[8])
    mixed = after_own + (own + sum(r9[d].astype(F32) for d in range(1, 8)))
    out_ref[...] = pltpu.roll(mixed, (4 - tp % 4) % 4 * 32, axis=1)[:, 0:32].astype(BF16)

    for phase, ref in enumerate([
        g1.at[pl.ds(0, 7)], r2.at[pl.ds(0, 120)], a3.at[pl.ds(0, 15)], r4.at[pl.ds(0, 240)], a5.at[pl.ds(0, 15)],
        a6.at[pl.ds(0, 7)], r7.at[pl.ds(0, 360)], a8.at[pl.ds(0, 15)], r9.at[pl.ds(0, 7)], g1m.at[pl.ds(0, 7)],
    ]):
        wait_bytes(ref, send_sem.at[phase])


def per_device(hidden_in, attn_gain, query_weight, key_cache, value_cache, lambdas, head_gain, out_weight,
               mixer_gain, gate_weight, up_weight, down_weight):
    args = (
        hidden_in, attn_gain.reshape(1, 256), query_weight, key_cache.reshape(16, 1024, 128), value_cache.reshape(16, 1024, 128),
        lambdas.reshape(1, 4), head_gain.reshape(1, 128), out_weight, mixer_gain.reshape(1, 32), gate_weight, up_weight, down_weight,
    )
    V = pltpu.VMEM
    return pl.pallas_call(
        kernel,
        name="layer",
        out_shape=jax.ShapeDtypeStruct((16, 32), BF16),
        in_specs=[pl.BlockSpec(memory_space=pl.ANY)] * len(args),
        out_specs=pl.BlockSpec(memory_space=pltpu.VMEM),
        scratch_shapes=[
            *(V(a.shape, a.dtype) for a in args),
            V((8, 16, 128), BF16), V((8, 1, 128), F32),
            V((128, 128), F32), V((128, 128), F32), V((16, 8, 128), BF16),
            V((256, 128), F32), V((256, 128), F32), V((16, 8, 128), BF16), V((128, 128), F32),
            V((8, 16, 256), BF16),
            V((384, 128), F32), V((384, 128), F32), V((16, 16, 128), BF16), V((256, 128), F32),
            V((2, 16, 128), BF16), V((8, 16, 128), BF16),
            pltpu.SemaphoreType.DMA((12,)), pltpu.SemaphoreType.DMA((10,)), pltpu.SemaphoreType.DMA((10,)),
        ],
        compiler_params=pltpu.CompilerParams(collective_id=0, has_side_effects=True, vmem_limit_bytes=48 * 2**20),
    )(*args)


def solution(mesh):
    placed = (
        P(None, ("kv", "tp")), P("kv"), P("kv", "tp"), P(None, "kv", "tp", None), P(None, "kv", "tp", None), P("tp"),
        P(), P("tp", "kv"), P(("kv", "tp")), P("kv", "tp"), P("kv", "tp"), P("tp", "kv"),
    )
    return jax.shard_map(per_device, mesh=mesh, in_specs=placed, out_specs=P(None, ("kv", "tp")), check_vma=False)
```
